32 devices in a mesh: sp: 8 (over z, x), tp: 4 (over y, core).
Axes of the slice: x: 2, y: 2, z: 4, core: 2. Of those that a mesh axis runs over, the one named last changes fastest.
Arguments:
- residual_in: bfloat16 [8192, 2048], P(('sp', 'tp')), may hold values from -6 to 6
- gate_outer: bfloat16 [8192, 1024], P('sp', 'tp'), may hold values from -6 to 6
- gate_inner: bfloat16 [8192, 1024], P('sp', 'tp'), may hold values from -6 to 6
- conv_input: bfloat16 [8192, 1024], P('sp', 'tp'), may hold values from -6 to 6
- conv_taps: bfloat16 [3, 1024], P(None, 'tp'), may hold values from -5 to 5
- norm_gain: bfloat16 [1024], P('tp'), may hold values from 0.099609375 to 1.8984375
- out_weight: bfloat16 [1024, 2048], P('tp'), may hold values from -0.1875 to 0.1875
- moe_gain: bfloat16 [2048], replicated, may hold values from 0.099609375 to 1.8984375
- expert_ids: int32 [8192, 2], P(('sp', 'tp')), may hold values from 0 to 7, all different within a row; in each aligned block of 256 rows (0 to 255, 256 to 511, ...) at most 128 rows name the same one
- group_prob: float32 [8192], P(('sp', 'tp')), may hold values from 0.3 to 1
- route_prob: float32 [8192, 2], P(('sp', 'tp')), may hold values from 0.1 to 1
- expert_gate: bfloat16 [8, 2048, 512], P('sp'), may hold values from -0.125 to 0.125
- expert_up: bfloat16 [8, 2048, 512], P('sp'), may hold values from -0.125 to 0.125
- expert_down: bfloat16 [8, 512, 2048], P('sp'), may hold values from -0.25 to 0.25
Outputs:
- layer_out: bfloat16 [8192, 2048], P(('sp', 'tp'))
The draws below stay inside these ranges and needn't reach their ends.
Inputs may be any that keep to these rules, and one draw needn't show every extreme that they name: `expert_ids`: each row names 2 different experts. Within the rows of one device (aligned blocks of 256 rows) no expert is named more than 128 times.
All inputs are finite; a program needn't handle non-finite values.
Results may differ from the reference program's by a relative error of at most 0.0075.
Values may be sent and summed in bfloat16 or wider, within the bound.
A program may use at most 64 MiB of HBM per device.

```python
import math
import jax
import jax.numpy as jnp
import numpy as np
from jax import lax

D = 2048
CONV = 1024
FE = 512
KW = 3
TOPK = 2
ROWS_DEV = 256
TOKENS = 8192
EXPERTS = 8
CAPACITY = 128


def draw_conv_taps(key, part):
    first, second = jax.random.split(key)
    base = jnp.clip(jax.random.normal(first, (KW, CONV), jnp.float32), -3.0, 3.0) / jnp.sqrt(jnp.float32(KW))
    levels = jnp.array([0.35, 0.7, 1.4, 2.8], jnp.float32)
    shuffled = levels[jax.random.permutation(second, 4)]
    quarter = jnp.arange(CONV, dtype=jnp.int32) * 4 // CONV
    return (base * shuffled[quarter][None, :]).astype(jnp.bfloat16)


def shard_levels(stream_key, extent, pieces, low, high):
    factor_of, own = 1.0, jax.random.fold_in(stream_key, 6)
    for position, blocks in pieces:
        steps = jnp.exp(jax.random.uniform(jax.random.fold_in(own, position), (blocks,), jnp.float32, low / len(pieces), high / len(pieces)))
        factor_of = factor_of * jnp.repeat(steps, extent[position] // blocks).reshape([-1 if axis == position else 1 for axis in range(len(extent))])
    return factor_of


def assign_block(key, own, number, rows, number_of, top, reach, slope):
    ranking = jax.random.permutation(key, number_of)
    heavy_load, common = shares(number_of, rows * top, reach, slope, True), shares(number_of, rows * top, reach, slope, False)
    places = jnp.arange(number_of)

    def named(sizes, turn):
        used = int((sizes > 0).sum())
        fixed = max(1, used // 4)
        moved = fixed + (places - fixed + turn * (used - fixed)) % max(1, number_of - fixed)
        return jnp.zeros((number_of,), jnp.int32).at[ranking[jnp.where(places < fixed, places, moved)]].set(jnp.asarray(sizes, jnp.int32))

    sizes = jnp.where(number % 4 == 0, named(heavy_load, number // 4), named(common, number - number // 4 - 1))
    mixed = jax.random.permutation(jax.random.fold_in(own, 3), number_of)
    donor, receiver = mixed[0:number_of // 2 * 2:2], mixed[1:number_of // 2 * 2:2]
    margin = jnp.minimum(sizes[donor] - 1, reach - sizes[receiver]) // 2
    margin = jnp.where((donor == ranking[0]) | (receiver == ranking[0]) | (sizes[receiver] == 0), 0, jnp.maximum(margin, 0))
    moved = jax.random.randint(jax.random.fold_in(own, 4), (number_of // 2,), 0, 1 << 20) % (margin + 1)
    sizes = sizes.at[donor].add(-moved).at[receiver].add(moved)
    items = jnp.searchsorted(jnp.cumsum(sizes), jnp.arange(rows * top), side="right").astype(jnp.int32)
    listing = items.reshape(top, rows).T
    listing = listing[jax.random.permutation(jax.random.fold_in(own, 1), rows)]
    turn = jax.random.randint(jax.random.fold_in(own, 2), (rows, 1), 0, top)
    return jnp.take_along_axis(listing, (jnp.arange(top)[None, :] + turn) % top, axis=1)


def shares(count, total, reach, slope, full):
    loads = [(1 << 20) // math.isqrt(rank ** slope) + 1 for rank in range(1, count + 1)]
    largest = reach if full else min(reach, max(-(-total // count), total * loads[0] // sum(loads)))
    least = 1 if total - largest >= count - 1 else 0
    holding, rest = [largest] + [least] * (count - 1), total - largest - least * (count - 1)
    while rest > 0:
        candidates = [i for i in range(1, count) if holding[i] < largest] or [i for i in range(1, count) if holding[i] < reach]
        pool, left = sum([loads[i] for i in candidates]), rest
        for i in candidates:
            more = min(reach - holding[i], max(1, left * loads[i] // pool), rest)
            holding[i] = holding[i] + more
            rest = rest - more
    return np.array(holding)


def normal_values(stream_key, dims, deviation, most, cuts=(), kind=jnp.bfloat16):
    values = jax.random.normal(stream_key, dims, jnp.float32) * deviation
    if len(cuts) > 0:
        values = shard_levels(stream_key, dims, cuts, -0.22, 0.18) * values
    return jnp.clip(values, min=-most, max=most).astype(kind)


def setup_inputs(seed: int = 0) -> dict:
    key_list = jax.random.split(jax.random.key(seed), 15)
    residual_in = normal_values(key_list[0], (TOKENS, D), 1.0, 6.0, ((0, 32),))
    gate_outer = normal_values(key_list[1], (TOKENS, CONV), 1.0, 6.0, ((0, 8), (1, 4)))
    gate_inner = normal_values(key_list[2], (TOKENS, CONV), 1.0, 6.0, ((0, 8), (1, 4)))
    conv_input = normal_values(key_list[3], (TOKENS, CONV), 1.0, 6.0, ((0, 8), (1, 4)))
    conv_taps = draw_conv_taps(jax.random.fold_in(key_list[14], 71), 0)
    norm_gain = jnp.clip(1.0 + 0.18 * jax.random.normal(key_list[5], (CONV,), jnp.float32), 0.099609375, 1.8984375).astype(jnp.bfloat16)
    out_weight = normal_values(key_list[6], (CONV, D), CONV ** -0.5, 0.1875, ((0, 4),))
    moe_gain = jnp.clip(1.0 + 0.18 * jax.random.normal(key_list[7], (D,), jnp.float32), 0.099609375, 1.8984375).astype(jnp.bfloat16)
    expert_ids_keys = jax.random.split(jax.random.fold_in(key_list[8], 1), TOKENS // ROWS_DEV)
    expert_ids_turns = jax.random.permutation(jax.random.fold_in(key_list[8], 3), TOKENS // ROWS_DEV)
    expert_ids = jax.vmap(lambda own, number: assign_block(jax.random.fold_in(key_list[8], 2), own, number, ROWS_DEV, EXPERTS, TOPK, CAPACITY, 2))(expert_ids_keys, expert_ids_turns).reshape((TOKENS, TOPK))
    group_prob = jnp.clip(0.3 + 0.7 * jax.random.uniform(key_list[9], (TOKENS,), jnp.float32) ** shard_levels(key_list[9], (TOKENS,), ((0, 32),), -0.2, 0.2), 0.3, 1.0)
    route_prob = jnp.clip(0.1 + 0.9 * jax.random.uniform(key_list[10], (TOKENS, TOPK), jnp.float32) ** shard_levels(key_list[10], (TOKENS, TOPK), ((0, 32),), -0.2, 0.2), 0.1, 1.0)
    expert_gate = normal_values(key_list[11], (EXPERTS, D, FE), D ** -0.5, 0.125, ((0, 8),))
    expert_up = normal_values(key_list[12], (EXPERTS, D, FE), D ** -0.5, 0.125, ((0, 8),))
    expert_down = normal_values(key_list[13], (EXPERTS, FE, D), FE ** -0.5, 0.25, ((0, 8),))
    return dict(residual_in=residual_in, gate_outer=gate_outer, gate_inner=gate_inner, conv_input=conv_input, conv_taps=conv_taps, norm_gain=norm_gain, out_weight=out_weight, moe_gain=moe_gain, expert_ids=expert_ids, group_prob=group_prob, route_prob=route_prob, expert_gate=expert_gate, expert_up=expert_up, expert_down=expert_down)


EPSILON = 1e-06

def rms_norm(values, gain):
    floats = values.astype(jnp.float32)
    factor = lax.rsqrt(lax.optimization_barrier(jnp.mean(floats * floats, axis=-1, keepdims=True)) + EPSILON)
    return floats * factor * gain.astype(jnp.float32)

def reference(residual_in, gate_outer, gate_inner, conv_input, conv_taps, norm_gain, out_weight, moe_gain, expert_ids, group_prob, route_prob, expert_gate, expert_up, expert_down):
    inner = gate_inner.astype(jnp.float32) * conv_input.astype(jnp.float32)
    padded = jnp.concatenate([jnp.zeros((KW - 1, CONV), jnp.float32), inner], axis=0)
    tap_f = conv_taps.astype(jnp.float32)
    filtered = jnp.zeros((TOKENS, CONV), jnp.float32)
    for offset in range(KW):
        filtered = filtered + tap_f[offset][None, :] * padded[offset:offset + TOKENS]
    mixed = (gate_outer.astype(jnp.float32) * filtered).astype(jnp.bfloat16)
    normed = rms_norm(mixed, norm_gain).astype(jnp.bfloat16)
    residual = (residual_in.astype(jnp.float32) + jnp.dot(normed, out_weight, preferred_element_type=jnp.float32)).astype(jnp.bfloat16)
    routed_in = rms_norm(residual, moe_gain).astype(jnp.bfloat16)
    slots = TOKENS * TOPK
    block_rows = 256
    flat_e = expert_ids.reshape(-1).astype(jnp.int32)
    order = jnp.argsort(flat_e, stable=True).astype(jnp.int32)
    sorted_e = flat_e[order]
    counts = jnp.bincount(flat_e, length=EXPERTS).astype(jnp.int32)
    padded_counts = (counts + block_rows - 1) // block_rows * block_rows
    pad_end = jnp.cumsum(padded_counts).astype(jnp.int32)
    pad_start = pad_end - padded_counts
    seg_start = (jnp.cumsum(counts) - counts).astype(jnp.int32)
    dest = pad_start[sorted_e] + jnp.arange(slots, dtype=jnp.int32) - seg_start[sorted_e]
    block_count = (slots + block_rows - 1) // block_rows + EXPERTS
    total_rows = block_count * block_rows
    buffer_slot = jnp.full((total_rows,), slots, jnp.int32).at[dest].set(order)
    block_expert = jnp.minimum(jnp.searchsorted(pad_end, jnp.arange(block_count, dtype=jnp.int32) * block_rows, side='right'), EXPERTS - 1).astype(jnp.int32)
    rows_pad = jnp.concatenate([routed_in, jnp.zeros((1, D), jnp.bfloat16)], axis=0)

    def one_block(items):
        slot_ids, expert = items
        token_row = jnp.where(slot_ids < slots, slot_ids // TOPK, TOKENS)
        block_in = rows_pad[token_row]
        gate_act = jnp.dot(block_in, expert_gate[expert], preferred_element_type=jnp.float32)
        up_act = jnp.dot(block_in, expert_up[expert], preferred_element_type=jnp.float32)
        hidden = (jax.nn.silu(gate_act) * up_act).astype(jnp.bfloat16)
        return jnp.dot(hidden, expert_down[expert], preferred_element_type=jnp.float32).astype(jnp.bfloat16)
    results = lax.map(one_block, (buffer_slot.reshape(block_count, block_rows), block_expert)).reshape(total_rows, D)
    slot_out = jnp.zeros((slots + 1, D), jnp.bfloat16).at[buffer_slot].set(results)[:slots]
    weights = group_prob[:, None] * route_prob / lax.optimization_barrier(jnp.sum(route_prob, axis=1, keepdims=True))
    expert_sum = lax.optimization_barrier(jnp.sum(slot_out.reshape(TOKENS, TOPK, D).astype(jnp.float32) * weights[:, :, None], axis=1))
    return (residual.astype(jnp.float32) + expert_sum).astype(jnp.bfloat16)
```

```python
import functools
import jax
import jax.numpy as jnp
from jax import lax
from jax.experimental import pallas as pl
from jax.experimental.pallas import tpu as pltpu
from jax.sharding import PartitionSpec as P

EPSILON = 1e-06


def from_behind(shard, axis, by):
    devices = lax.axis_size(axis)
    pairs = [(i, i + by) for i in range(devices) if 0 <= i + by < devices]
    return lax.ppermute(shard, axis, pairs)


def rms_norm(values, gain):
    floats = values.astype(jnp.float32)
    factor = lax.rsqrt(jnp.mean(floats * floats, axis=-1, keepdims=True) + EPSILON)
    return floats * factor * gain.astype(jnp.float32)


GATHER_BYTES = 26 * 2**20


def ffn_kernel(x_ref, w_ref, gate_ref, up_ref, down_ref, out_ref, acc_ref):
    step = pl.program_id(0)
    x = x_ref[...]
    gate = jnp.dot(x, gate_ref[0], preferred_element_type=jnp.float32)
    up = jnp.dot(x, up_ref[0], preferred_element_type=jnp.float32)
    hidden = (w_ref[0] * (jax.nn.silu(gate) * up)).astype(jnp.bfloat16)
    part = jnp.dot(hidden, down_ref[0], preferred_element_type=jnp.float32)

    @pl.when(step == 0)
    def _():
        acc_ref[...] = part

    @pl.when(step > 0)
    def _():
        acc_ref[...] += part

    @pl.when(step == pl.num_programs(0) - 1)
    def _():
        out_ref[...] = acc_ref[...].astype(out_ref.dtype)


def weighted_experts(x, w, gate, up, down, out_dtype):
    rows, width = x.shape
    pieces, _, units = gate.shape
    experts = w.shape[0]
    return pl.pallas_call(
        ffn_kernel,
        grid=(pieces,),
        in_specs=[
            pl.BlockSpec((rows, width), lambda g: (0, 0)),
            pl.BlockSpec((1, rows, 1), lambda g: (PIECE_EXPERT(g, experts, pieces), 0, 0)),
            pl.BlockSpec((1, width, units), lambda g: (g, 0, 0)),
            pl.BlockSpec((1, width, units), lambda g: (g, 0, 0)),
            pl.BlockSpec((1, units, width), lambda g: (g, 0, 0)),
        ],
        out_specs=pl.BlockSpec((rows, width), lambda g: (0, 0)),
        out_shape=jax.ShapeDtypeStruct((rows, width), out_dtype),
        scratch_shapes=[pltpu.VMEM((rows, width), jnp.float32)],
        compiler_params=pltpu.CompilerParams(dimension_semantics=("arbitrary",), vmem_limit_bytes=40 * 2**20),
        cost_estimate=pl.CostEstimate(
            flops=6 * rows * width * units * pieces,
            bytes_accessed=6 * pieces * width * units + 6 * rows * width,
            transcendentals=rows * units * pieces,
        ),
    )(x, w, gate, up, down)


def PIECE_EXPERT(g, experts, pieces):
    return g // (pieces // experts)


def half_slice(residual, routed_in, ids, group_prob, route_prob, gate, up, down):
    sp, tp = lax.axis_size("sp"), lax.axis_size("tp")
    half = sp // 2
    local = gate.shape[0]
    rows, width = routed_in.shape
    tp_me, sp_me = lax.axis_index("tp"), lax.axis_index("sp")
    units = gate.shape[2] // tp
    gate_cut = lax.dynamic_slice_in_dim(gate, tp_me * units, units, 2)
    up_cut = lax.dynamic_slice_in_dim(up, tp_me * units, units, 2)
    down_cut = lax.dynamic_slice_in_dim(down, tp_me * units, units, 1)
    groups = [[(h * half + s) * tp + t for s in range(half) for t in range(tp)] for h in range(2)]
    gather = functools.partial(
        lax.all_gather, axis_name=("sp", "tp"), axis_index_groups=groups, axis=0, tiled=True
    )
    gates, ups, downs = gather(gate_cut), gather(up_cut), gather(down_cut)
    experts_half = local * half
    assert local == 1
    pairs = [(i, (i + half) % sp) for i in range(sp)]
    weights = group_prob[:, None] * route_prob / jnp.sum(route_prob, axis=1, keepdims=True)
    dense = jnp.sum(
        jnp.where(
            ids[None, :, :] == jnp.arange(experts_half * 2, dtype=jnp.int32)[:, None, None],
            weights[None],
            0.0,
        ),
        axis=2,
    ).reshape(2, experts_half, rows)
    mine = lax.dynamic_index_in_dim(dense, sp_me // half, 0, keepdims=False)[:, :, None]
    other = lax.dynamic_index_in_dim(dense, 1 - sp_me // half, 0, keepdims=False)
    other = lax.ppermute(other, "sp", pairs)[:, :, None]
    across = lax.ppermute(routed_in, "sp", pairs)
    own = weighted_experts(routed_in, mine, gates, ups, downs, jnp.float32)
    theirs = weighted_experts(across, other, gates, ups, downs, jnp.bfloat16)
    back = lax.ppermute(theirs, "sp", pairs)
    return (residual.astype(jnp.float32) + own + back.astype(jnp.float32)).astype(jnp.bfloat16)


def exchange_slots(residual, routed_in, expert_ids, group_prob, route_prob, expert_gate, expert_up, expert_down):
    tok_rows, width = routed_in.shape
    top_count = expert_ids.shape[1]
    local_count = expert_gate.shape[0]
    group_count = lax.axis_size("sp")
    experts_all = local_count * group_count
    capacity = 2 * tok_rows * top_count // experts_all
    slots = tok_rows * top_count
    flat_e = expert_ids.reshape(-1)
    one_hot = (flat_e[:, None] == jnp.arange(experts_all, dtype=jnp.int32)[None, :]).astype(
        jnp.int32
    )
    slot_rank = jnp.sum((jnp.cumsum(one_hot, axis=0) - 1) * one_hot, axis=1)
    owner_dev = flat_e // local_count
    local_slot = flat_e % local_count
    position = (local_slot * group_count + owner_dev) * capacity + slot_rank
    source_slot = (
        jnp.full((experts_all * capacity,), slots, jnp.int32)
        .at[position]
        .set(jnp.arange(slots, dtype=jnp.int32))
    )
    rows_pad = jnp.concatenate([routed_in, jnp.zeros((1, width), jnp.bfloat16)], axis=0)
    outgoing = rows_pad[source_slot // top_count].reshape(local_count, group_count, capacity, width)
    arrived = lax.all_to_all(outgoing, "sp", split_axis=1, concat_axis=1, tiled=True)
    gate_act = jnp.einsum(
        "esrd,edf->esrf", arrived, expert_gate, preferred_element_type=jnp.float32
    )
    up_act = jnp.einsum("esrd,edf->esrf", arrived, expert_up, preferred_element_type=jnp.float32)
    hidden = (jax.nn.silu(gate_act) * up_act).astype(jnp.bfloat16)
    result = jnp.einsum(
        "esrf,efd->esrd", hidden, expert_down, preferred_element_type=jnp.float32
    ).astype(jnp.bfloat16)
    returned = lax.all_to_all(result, "sp", split_axis=1, concat_axis=1, tiled=True)
    slot_out = returned.reshape(-1, width)[position].reshape(tok_rows, top_count, width)
    weights = group_prob[:, None] * route_prob / jnp.sum(route_prob, axis=1, keepdims=True)
    expert_sum = jnp.sum(slot_out.astype(jnp.float32) * weights[:, :, None], axis=1)
    return (residual.astype(jnp.float32) + expert_sum).astype(jnp.bfloat16)


def body(
    residual_in,
    gate_outer,
    gate_inner,
    conv_input,
    conv_taps,
    norm_gain,
    out_weight,
    moe_gain,
    expert_ids,
    group_prob,
    route_prob,
    expert_gate,
    expert_up,
    expert_down,
):
    seq_rows, channels = conv_input.shape
    taps_count = conv_taps.shape[0]
    inner = gate_inner.astype(jnp.float32) * conv_input.astype(jnp.float32)
    earlier = from_behind(inner[seq_rows - (taps_count - 1) :], "sp", 1)
    padded = jnp.concatenate([earlier, inner], axis=0)
    tap_f = conv_taps.astype(jnp.float32)
    filtered = jnp.zeros((seq_rows, channels), jnp.float32)
    for offset in range(taps_count):
        filtered = filtered + tap_f[offset][None, :] * padded[offset : offset + seq_rows]
    mixed_out = (gate_outer.astype(jnp.float32) * filtered).astype(jnp.bfloat16)
    gathered = lax.all_to_all(mixed_out, "tp", split_axis=0, concat_axis=1, tiled=True)
    full_weight, full_gain = (
        lax.all_gather(out_weight, "tp", axis=0, tiled=True),
        lax.all_gather(norm_gain, "tp", axis=0, tiled=True),
    )
    normed = rms_norm(gathered, full_gain).astype(jnp.bfloat16)
    projected = jnp.dot(normed, full_weight, preferred_element_type=jnp.float32)
    residual = (residual_in.astype(jnp.float32) + projected).astype(jnp.bfloat16)
    routed_in = rms_norm(residual, moe_gain).astype(jnp.bfloat16)
    sp = lax.axis_size("sp")
    expert_bytes = 3 * expert_gate.size * expert_gate.dtype.itemsize
    fits = expert_gate.shape[0] == 1 and sp % 2 == 0 and expert_bytes * sp // 2 <= GATHER_BYTES
    experts = half_slice if fits else exchange_slots
    return experts(
        residual, routed_in, expert_ids, group_prob, route_prob, expert_gate, expert_up, expert_down
    )


def solution(mesh):
    in_specs = (
        P(("sp", "tp"), None),
        P("sp", "tp"),
        P("sp", "tp"),
        P("sp", "tp"),
        P(None, "tp"),
        P("tp"),
        P("tp", None),
        P(),
        P(("sp", "tp"), None),
        P(("sp", "tp")),
        P(("sp", "tp"), None),
        P("sp", None, None),
        P("sp", None, None),
        P("sp", None, None),
    )
    out_specs = P(("sp", "tp"), None)
    return jax.shard_map(body, mesh=mesh, in_specs=in_specs, out_specs=out_specs, check_vma=False)
```

```python
import functools
import jax
import jax.numpy as jnp
from jax import lax
from jax.experimental import pallas as pl
from jax.experimental.pallas import tpu as pltpu
from jax.sharding import PartitionSpec as P

EPSILON = 1e-06


def from_behind(shard, axis, by):
    devices = lax.axis_size(axis)
    pairs = [(i, i + by) for i in range(devices) if 0 <= i + by < devices]
    return lax.ppermute(shard, axis, pairs)


def rms_norm(values, gain):
    floats = values.astype(jnp.float32)
    factor = lax.rsqrt(jnp.mean(floats * floats, axis=-1, keepdims=True) + EPSILON)
    return floats * factor * gain.astype(jnp.float32)


GATHER_BYTES = 26 * 2**20
GAIN_ROWS = 16
HALO_ROWS = 8


def conv_kernel(outer_ref, inner_ref, input_ref, inner_back, input_back, halo_ref, taps_ref, gain_ref, out_ref):
    rows = outer_ref.shape[0]
    inner = inner_ref[...].astype(jnp.float32) * input_ref[...].astype(jnp.float32)
    behind = inner_back[...].astype(jnp.float32) * input_back[...].astype(jnp.float32)
    behind = behind[behind.shape[0] - HALO_ROWS :]
    behind = jnp.where(pl.program_id(0) == 0, halo_ref[...], behind)
    padded = jnp.concatenate([behind, inner], axis=0)
    taps = taps_ref[...].astype(jnp.float32)
    count = taps.shape[0]
    filtered = jnp.zeros_like(inner)
    for offset in range(count):
        first = HALO_ROWS - (count - 1) + offset
        filtered = filtered + taps[offset][None, :] * padded[first : first + rows]
    mixed = (outer_ref[...].astype(jnp.float32) * filtered).astype(jnp.bfloat16)
    out_ref[0, :rows] = mixed
    out_ref[0, rows:] = jnp.broadcast_to(gain_ref[...], (GAIN_ROWS, mixed.shape[1]))


def conv_blocks(outer, inner, values, halo, taps, gain, pieces):
    rows, channels = outer.shape
    block = rows // pieces
    back = 2 * HALO_ROWS
    main = pl.BlockSpec((block, channels), lambda b: (b, 0))
    before = pl.BlockSpec((back, channels), lambda b: (jnp.maximum(b * (block // back) - 1, 0), 0))
    whole = lambda a: pl.BlockSpec(a.shape, lambda b: (0, 0))
    return pl.pallas_call(
        conv_kernel,
        grid=(pieces,),
        in_specs=[main, main, main, before, before, whole(halo), whole(taps), whole(gain)],
        out_specs=pl.BlockSpec((1, block + GAIN_ROWS, channels), lambda b: (b, 0, 0)),
        out_shape=jax.ShapeDtypeStruct((pieces, block + GAIN_ROWS, channels), jnp.bfloat16),
        cost_estimate=pl.CostEstimate(
            flops=8 * rows * channels, bytes_accessed=8 * rows * channels, transcendentals=0
        ),
        compiler_params=pltpu.CompilerParams(vmem_limit_bytes=16 * 2**20),
    )(outer, inner, values, inner, values, halo, taps, gain)


def project_kernel(order, mixed_ref, *refs):
    count = mixed_ref.shape[0]
    weight_refs, (residual_ref, gain_ref, residual_out, routed_out) = refs[:count], refs[count:]
    rows = residual_ref.shape[0]
    channels = count * mixed_ref.shape[2]
    me = lax.axis_index("tp")
    total = jnp.zeros((rows, 1), jnp.float32)
    for step in range(count):
        block = mixed_ref[step, :rows].astype(jnp.float32)
        total = total + jnp.sum(block * block, axis=1, keepdims=True)
    factor = lax.rsqrt(total / channels + EPSILON)
    out = residual_ref[...].astype(jnp.float32)
    for step, weight_ref in zip(order, weight_refs):
        block = mixed_ref[me ^ step]
        gain = block[rows : rows + 1].astype(jnp.float32)
        normed = (block[:rows].astype(jnp.float32) * factor * gain).astype(jnp.bfloat16)
        out = out + jnp.dot(normed, weight_ref[...], preferred_element_type=jnp.float32)
    residual = out.astype(jnp.bfloat16)
    residual_out[...] = residual
    floats = residual.astype(jnp.float32)
    mean = jnp.mean(floats * floats, axis=1, keepdims=True)
    routed = floats * lax.rsqrt(mean + EPSILON) * gain_ref[...].astype(jnp.float32)
    routed_out[...] = routed.astype(jnp.bfloat16)


def project(mixed, weights, order, residual_in, gain):
    rows, width = residual_in.shape
    vmem = pl.BlockSpec(memory_space=pltpu.VMEM)
    shape = jax.ShapeDtypeStruct((rows, width), jnp.bfloat16)
    return pl.pallas_call(
        functools.partial(project_kernel, order),
        in_specs=[vmem] * (len(weights) + 3),
        out_specs=[vmem, vmem],
        out_shape=[shape, shape],
        cost_estimate=pl.CostEstimate(
            flops=2 * rows * width * mixed.shape[0] * mixed.shape[2],
            bytes_accessed=2 * width * mixed.shape[0] * mixed.shape[2] + 8 * rows * width,
            transcendentals=0,
        ),
        compiler_params=pltpu.CompilerParams(vmem_limit_bytes=32 * 2**20),
    )(mixed, *weights, residual_in, gain)


def ffn_kernel(x_ref, y_ref, wx_ref, wy_ref, both_ref, down_ref, x_out, y_out, x_acc, y_acc):
    step = pl.program_id(0)
    cuts, units, width = down_ref.shape
    down = down_ref[...].reshape(cuts * units, width)

    def part(rows_ref, w_ref):
        rows = rows_ref[...]
        hidden = []
        for cut in range(cuts):
            act = jnp.dot(rows, both_ref[cut], preferred_element_type=jnp.float32)
            gated = jax.nn.silu(act[:, :units]) * act[:, units:]
            hidden.append((w_ref[0] * gated).astype(jnp.bfloat16))
        hidden = jnp.concatenate(hidden, axis=1)
        return jnp.dot(hidden, down, preferred_element_type=jnp.float32)

    for rows_ref, w_ref, out_ref, acc_ref in (
        (x_ref, wx_ref, x_out, x_acc),
        (y_ref, wy_ref, y_out, y_acc),
    ):
        value = part(rows_ref, w_ref)

        @pl.when(step == 0)
        def _():
            acc_ref[...] = value

        @pl.when((step > 0) & (step < pl.num_programs(0) - 1))
        def _():
            acc_ref[...] += value

        @pl.when(step == pl.num_programs(0) - 1)
        def _():
            out_ref[...] = (acc_ref[...] + value).astype(out_ref.dtype)


def weighted_experts(x, y, wx, wy, both, down, x_dtype):
    rows, width = x.shape
    pieces, units, _ = down.shape
    experts = wx.shape[0]
    cuts = pieces // experts
    full = pl.BlockSpec((rows, width), lambda e: (0, 0))
    scale = pl.BlockSpec((1, rows, 1), lambda e: (e, 0, 0))
    return pl.pallas_call(
        ffn_kernel,
        grid=(experts,),
        in_specs=[
            full,
            full,
            scale,
            scale,
            pl.BlockSpec((cuts, width, 2 * units), lambda e: (e, 0, 0)),
            pl.BlockSpec((cuts, units, width), lambda e: (e, 0, 0)),
        ],
        out_specs=[full, full],
        out_shape=[
            jax.ShapeDtypeStruct((rows, width), x_dtype),
            jax.ShapeDtypeStruct((rows, width), jnp.bfloat16),
        ],
        scratch_shapes=[pltpu.VMEM((rows, width), jnp.float32)] * 2,
        compiler_params=pltpu.CompilerParams(
            dimension_semantics=("arbitrary",), vmem_limit_bytes=40 * 2**20
        ),
        cost_estimate=pl.CostEstimate(
            flops=12 * rows * width * units * pieces,
            bytes_accessed=6 * pieces * width * units + 12 * rows * width,
            transcendentals=2 * rows * units * pieces,
        ),
    )(x, y, wx, wy, both, down)


def half_slice(
    residual_in,
    gate_outer,
    gate_inner,
    conv_input,
    conv_taps,
    norm_gain,
    out_weight,
    moe_gain,
    expert_ids,
    group_prob,
    route_prob,
    expert_gate,
    expert_up,
    expert_down,
):
    sp, tp = lax.axis_size("sp"), lax.axis_size("tp")
    half, lanes = sp // 2, tp // 2
    sp_me, tp_me = lax.axis_index("sp"), lax.axis_index("tp")
    rows, width = residual_in.shape
    core = [(i, i ^ 1) for i in range(tp)]
    cross = [(i, (i + half) % sp) for i in range(sp)]

    weights, order = [out_weight], [0]
    for line in range(1, lanes):
        pairs = [(i, i ^ (2 * line)) for i in range(tp)]
        weights.append(lax.ppermute(out_weight, "tp", pairs))
        order.append(2 * line)
    weights += [lax.ppermute(block, "tp", core) for block in weights]
    order += [step ^ 1 for step in order]

    units = expert_gate.shape[2] // tp
    first = ((tp_me % 2) * lanes + tp_me // 2) * units
    gate_cut = lax.dynamic_slice_in_dim(expert_gate, first, units, 2)
    up_cut = lax.dynamic_slice_in_dim(expert_up, first, units, 2)
    down_cut = lax.dynamic_slice_in_dim(expert_down, first, units, 1)
    groups = [
        [(h * half + s) * tp + 2 * line + c for s in range(half) for line in range(lanes)]
        for h in range(2)
        for c in range(2)
    ]
    gather = functools.partial(
        lax.all_gather, axis_name=("sp", "tp"), axis_index_groups=groups, axis=0, tiled=True
    )
    both = gather(jnp.concatenate([gate_cut, up_cut], axis=2))
    down = gather(down_cut)

    scale = group_prob[:, None] * route_prob / jnp.sum(route_prob, axis=1, keepdims=True)
    experts = jnp.arange(sp, dtype=jnp.int32)[:, None, None]
    dense = jnp.sum(jnp.where(expert_ids[None] == experts, scale[None], 0.0), axis=2)
    pair = jnp.stack([dense, lax.ppermute(dense, "tp", core)]).reshape(2, 2, half, rows)
    pick = lambda h: lax.dynamic_index_in_dim(pair, h, 1, keepdims=False)
    near = pick(sp_me // half)[..., None]
    far = lax.ppermute(pick(1 - sp_me // half), "sp", cross)[..., None]

    taps = conv_taps.shape[0]
    tail = gate_inner[-HALO_ROWS:].astype(jnp.float32) * conv_input[-HALO_ROWS:].astype(jnp.float32)
    halo = from_behind(tail, "sp", 1)
    mixed = conv_blocks(gate_outer, gate_inner, conv_input, halo, conv_taps, norm_gain[None], tp)
    mixed = lax.all_to_all(mixed, "tp", split_axis=0, concat_axis=0, tiled=True)
    residual, routed = project(mixed, weights, order, residual_in, moe_gain[None])

    across = lax.ppermute(routed, "sp", cross)
    beside = lax.ppermute(routed, "tp", core)
    own, partner = weighted_experts(routed, beside, near[0], near[1], both, down, jnp.float32)
    across_beside = lax.ppermute(across, "tp", core)
    theirs, others = weighted_experts(
        across, across_beside, far[0], far[1], both, down, jnp.float32
    )
    theirs = (theirs + lax.ppermute(others, "tp", core).astype(jnp.float32)).astype(jnp.bfloat16)
    back = lax.ppermute(theirs, "sp", cross)
    own = own + lax.ppermute(partner, "tp", core).astype(jnp.float32)
    return (residual.astype(jnp.float32) + own + back.astype(jnp.float32)).astype(jnp.bfloat16)


def exchange_slots(
    residual_in,
    gate_outer,
    gate_inner,
    conv_input,
    conv_taps,
    norm_gain,
    out_weight,
    moe_gain,
    expert_ids,
    group_prob,
    route_prob,
    expert_gate,
    expert_up,
    expert_down,
):
    seq_rows, channels = conv_input.shape
    taps_count = conv_taps.shape[0]
    inner = gate_inner.astype(jnp.float32) * conv_input.astype(jnp.float32)
    earlier = from_behind(inner[seq_rows - (taps_count - 1) :], "sp", 1)
    padded = jnp.concatenate([earlier, inner], axis=0)
    tap_f = conv_taps.astype(jnp.float32)
    filtered = jnp.zeros((seq_rows, channels), jnp.float32)
    for offset in range(taps_count):
        filtered = filtered + tap_f[offset][None, :] * padded[offset : offset + seq_rows]
    mixed_out = (gate_outer.astype(jnp.float32) * filtered).astype(jnp.bfloat16)
    gathered = lax.all_to_all(mixed_out, "tp", split_axis=0, concat_axis=1, tiled=True)
    full_weight, full_gain = (
        lax.all_gather(out_weight, "tp", axis=0, tiled=True),
        lax.all_gather(norm_gain, "tp", axis=0, tiled=True),
    )
    normed = rms_norm(gathered, full_gain).astype(jnp.bfloat16)
    projected = jnp.dot(normed, full_weight, preferred_element_type=jnp.float32)
    residual = (residual_in.astype(jnp.float32) + projected).astype(jnp.bfloat16)
    routed_in = rms_norm(residual, moe_gain).astype(jnp.bfloat16)
    tok_rows, width = routed_in.shape
    top_count = expert_ids.shape[1]
    local_count = expert_gate.shape[0]
    group_count = lax.axis_size("sp")
    experts_all = local_count * group_count
    capacity = 2 * tok_rows * top_count // experts_all
    slots = tok_rows * top_count
    flat_e = expert_ids.reshape(-1)
    one_hot = (flat_e[:, None] == jnp.arange(experts_all, dtype=jnp.int32)[None, :]).astype(
        jnp.int32
    )
    slot_rank = jnp.sum((jnp.cumsum(one_hot, axis=0) - 1) * one_hot, axis=1)
    owner_dev = flat_e // local_count
    local_slot = flat_e % local_count
    position = (local_slot * group_count + owner_dev) * capacity + slot_rank
    source_slot = (
        jnp.full((experts_all * capacity,), slots, jnp.int32)
        .at[position]
        .set(jnp.arange(slots, dtype=jnp.int32))
    )
    rows_pad = jnp.concatenate([routed_in, jnp.zeros((1, width), jnp.bfloat16)], axis=0)
    outgoing = rows_pad[source_slot // top_count].reshape(local_count, group_count, capacity, width)
    arrived = lax.all_to_all(outgoing, "sp", split_axis=1, concat_axis=1, tiled=True)
    gate_act = jnp.einsum(
        "esrd,edf->esrf", arrived, expert_gate, preferred_element_type=jnp.float32
    )
    up_act = jnp.einsum("esrd,edf->esrf", arrived, expert_up, preferred_element_type=jnp.float32)
    hidden = (jax.nn.silu(gate_act) * up_act).astype(jnp.bfloat16)
    result = jnp.einsum(
        "esrf,efd->esrd", hidden, expert_down, preferred_element_type=jnp.float32
    ).astype(jnp.bfloat16)
    returned = lax.all_to_all(result, "sp", split_axis=1, concat_axis=1, tiled=True)
    slot_out = returned.reshape(-1, width)[position].reshape(tok_rows, top_count, width)
    weights = group_prob[:, None] * route_prob / jnp.sum(route_prob, axis=1, keepdims=True)
    expert_sum = jnp.sum(slot_out.astype(jnp.float32) * weights[:, :, None], axis=1)
    return (residual.astype(jnp.float32) + expert_sum).astype(jnp.bfloat16)


def solution(mesh):
    in_specs = (
        P(("sp", "tp"), None),
        P("sp", "tp"),
        P("sp", "tp"),
        P("sp", "tp"),
        P(None, "tp"),
        P("tp"),
        P("tp", None),
        P(),
        P(("sp", "tp"), None),
        P(("sp", "tp")),
        P(("sp", "tp"), None),
        P("sp", None, None),
        P("sp", None, None),
        P("sp", None, None),
    )
    out_specs = P(("sp", "tp"), None)
    def body(*args):
        gate, outer = args[11], args[1]
        sp, tp = mesh.shape["sp"], mesh.shape["tp"]
        gathered = 3 * gate.size * gate.dtype.itemsize * sp // 4
        pairs = gate.shape[0] == 1 and sp % 2 == 0 and tp & (tp - 1) == 0 and tp > 1
        sized = gate.shape[2] % (128 * tp) == 0 and outer.shape[0] % (16 * tp) == 0
        if pairs and sized and gathered <= GATHER_BYTES:
            return half_slice(*args)
        return exchange_slots(*args)

    return jax.shard_map(body, mesh=mesh, in_specs=in_specs, out_specs=out_specs, check_vma=False)
```

```python
import functools
import jax
import jax.numpy as jnp
from jax import lax
from jax.experimental import pallas as pl
from jax.experimental.pallas import tpu as pltpu
from jax.sharding import PartitionSpec as P

MESH = pl.DeviceIdType.MESH
EPSILON = 1e-06


def from_behind(shard, axis, by):
    devices = lax.axis_size(axis)
    pairs = [(i, i + by) for i in range(devices) if 0 <= i + by < devices]
    return lax.ppermute(shard, axis, pairs)


def rms_norm(values, gain):
    floats = values.astype(jnp.float32)
    factor = lax.rsqrt(jnp.mean(floats * floats, axis=-1, keepdims=True) + EPSILON)
    return floats * factor * gain.astype(jnp.float32)


GATHER_BYTES = 26 * 2**20
GAIN_ROWS = 16
HALO_ROWS = 16


def mixer_kernel(
    outer_ref, inner_ref, input_ref, taps_ref, gain_ref, weight_ref, residual_ref, moe_ref, near_ref, far_ref,
    both_ref, down_ref,
    residual_out, routed_out, across_out, beside_out, across_beside_out,
    near_beside_out, far_out, far_beside_out, both_out, down_out,
    halo, sent, got, weights, send_sem, recv_sem,
):
    sp, tp = lax.axis_index("sp"), lax.axis_index("tp")
    sp_size, tp_size = lax.axis_size("sp"), lax.axis_size("tp")
    core_bit = 1 - 2 * (tp % 2)
    line_bit = 2 - 4 * ((tp // 2) % 2)
    lanes = [tp, tp + core_bit, tp + line_bit, tp + line_bit + core_bit]
    core, line = (sp, lanes[1]), (sp, lanes[2])
    x_peer = (sp + 1 - 2 * (sp % 2), tp)
    z_peer = (sp + 2 - 4 * ((sp // 2) % 2), tp)
    cross = ((sp + sp_size // 2) % sp_size, tp)
    after, before = ((sp + 1) % sp_size, tp), ((sp + sp_size - 1) % sp_size, tp)
    peers = [core, line, (sp, lanes[3]), x_peer, z_peer, cross, after, before]

    barrier = pltpu.get_barrier_semaphore()
    for peer in peers:
        pl.semaphore_signal(barrier, inc=1, device_id=peer, device_id_type=MESH)
    pl.semaphore_wait(barrier, len(peers))

    started = []

    def send(source, target, peer):
        number = len(started)
        copy = pltpu.make_async_remote_copy(
            src_ref=source, dst_ref=target, send_sem=send_sem.at[number], recv_sem=recv_sem.at[number],
            device_id=peer, device_id_type=MESH,
        )
        copy.start()
        started.append(copy)
        return copy

    full = inner_ref.shape[0]
    halos = [
        send(inner_ref.at[pl.ds(full - HALO_ROWS, HALO_ROWS)], halo.at[0], after),
        send(input_ref.at[pl.ds(full - HALO_ROWS, HALO_ROWS)], halo.at[1], after),
    ]
    weight_line = send(weight_ref, weights.at[1], line)
    weight_core = send(weight_ref, weights.at[0], core)

    def pieces(source_both, source_down, slot, piece, peer):
        return [
            send(source_both, both_out.at[slot, piece], peer),
            send(source_down, down_out.at[slot, piece], peer),
        ]

    x_first = pieces(both_ref.at[0], down_ref.at[0], 0, 0, x_peer)
    z_first = pieces(both_ref.at[1], down_ref.at[1], 1, 1, z_peer)
    x_second = pieces(both_ref.at[1], down_ref.at[1], 0, 1, x_peer)
    z_second = pieces(both_ref.at[0], down_ref.at[0], 1, 0, z_peer)
    near_copy = send(near_ref, near_beside_out, core)
    far_copy = send(far_ref, far_out, cross)

    for copy in halos:
        copy.wait_recv()
    rows = residual_ref.shape[0]
    taps = taps_ref[...].astype(jnp.float32)
    count = taps.shape[0]
    exchanged = []
    for step in (2, 3, 1, 0):
        block = lanes[step]
        first = pl.multiple_of(block * rows, rows)
        inner = inner_ref[pl.ds(first, rows)].astype(jnp.float32) * input_ref[pl.ds(first, rows)].astype(jnp.float32)
        back = pl.multiple_of(jnp.maximum(block * rows - HALO_ROWS, 0), HALO_ROWS)
        behind = inner_ref[pl.ds(back, HALO_ROWS)].astype(jnp.float32) * input_ref[pl.ds(back, HALO_ROWS)].astype(jnp.float32)
        outside = halo[0].astype(jnp.float32) * halo[1].astype(jnp.float32)
        outside = jnp.where(sp == 0, 0.0, outside)
        behind = jnp.where(block == 0, outside, behind)
        padded = jnp.concatenate([behind, inner], axis=0)
        filtered = jnp.zeros_like(inner)
        for offset in range(count):
            start = HALO_ROWS - (count - 1) + offset
            filtered = filtered + taps[offset][None, :] * padded[start : start + rows]
        mixed = (outer_ref[pl.ds(first, rows)].astype(jnp.float32) * filtered).astype(jnp.bfloat16)
        sent[step, :rows] = mixed
        sent[step, rows:] = jnp.broadcast_to(gain_ref[...], (GAIN_ROWS, mixed.shape[1]))
        if step > 0:
            exchanged.append(send(sent.at[step], got.at[step - 1], (sp, block)))

    for copy in exchanged:
        copy.wait_recv()
    blocks = [sent.at[0], got.at[0], got.at[1], got.at[2]]
    total = jnp.zeros((rows, 1), jnp.float32)
    for block in blocks:
        values = block[:rows].astype(jnp.float32)
        total = total + jnp.sum(values * values, axis=1, keepdims=True)
    factor = lax.rsqrt(total / (tp_size * inner_ref.shape[1]) + EPSILON)

    def normed(block):
        gain = block[rows:][:1].astype(jnp.float32)
        return (block[:rows].astype(jnp.float32) * factor * gain).astype(jnp.bfloat16)

    weight_line.wait_recv()
    weight_both = send(weights.at[1], weights.at[2], core)
    far_copy.wait_recv()
    far_beside = send(far_out, far_beside_out, core)
    weight_core.wait_recv()
    width = residual_ref.shape[1]
    out = residual_ref[...].astype(jnp.float32)
    out = out + jnp.dot(normed(blocks[0]), weight_ref[...], preferred_element_type=jnp.float32)
    out = out + jnp.dot(normed(blocks[1]), weights[0], preferred_element_type=jnp.float32)
    out = out + jnp.dot(normed(blocks[2]), weights[1], preferred_element_type=jnp.float32)
    weight_both.wait_recv()
    out = out + jnp.dot(normed(blocks[3]), weights[2], preferred_element_type=jnp.float32)
    residual = out.astype(jnp.bfloat16)
    residual_out[...] = residual
    floats = residual.astype(jnp.float32)
    mean = jnp.mean(floats * floats, axis=1, keepdims=True)
    routed = floats * lax.rsqrt(mean + EPSILON) * moe_ref[...].astype(jnp.float32)
    routed_out[...] = routed.astype(jnp.bfloat16)

    across = send(routed_out, across_out, cross)
    beside = send(routed_out, beside_out, core)
    for copy in x_first:
        copy.wait_recv()
    diagonal = pieces(both_out.at[0, 0], down_out.at[0, 0], 2, 0, z_peer)
    for copy in z_first:
        copy.wait_recv()
    diagonal += pieces(both_out.at[1, 1], down_out.at[1, 1], 2, 1, x_peer)
    across.wait_recv()
    across_beside = send(across_out, across_beside_out, core)
    late = x_second + z_second + [near_copy, far_beside, beside, across_beside] + diagonal
    for copy in late:
        copy.wait_recv()
    for copy in started:
        copy.wait_send()


COPIES = 26


def mixer(outer, inner, values, taps, gain, weight, residual_in, moe_gain, near, far, both, down):
    rows, width = residual_in.shape
    channels = outer.shape[1]
    tp = lax.axis_size("tp")
    vmem = pl.BlockSpec(memory_space=pltpu.VMEM)
    hbm = pl.BlockSpec(memory_space=pl.ANY)
    tokens = jax.ShapeDtypeStruct((rows, width), jnp.bfloat16)
    scale = jax.ShapeDtypeStruct(near.shape, near.dtype)
    return pl.pallas_call(
        mixer_kernel,
        in_specs=[vmem] * 10 + [hbm] * 2,
        out_specs=[vmem, vmem, hbm, hbm, hbm, vmem, vmem, vmem, hbm, hbm],
        out_shape=[tokens] * 5
        + [scale] * 3
        + [jax.ShapeDtypeStruct((3,) + a.shape, a.dtype) for a in (both, down)],
        scratch_shapes=[
            pltpu.VMEM((2, HALO_ROWS, channels), jnp.bfloat16),
            pltpu.VMEM((tp, rows + GAIN_ROWS, channels), jnp.bfloat16),
            pltpu.VMEM((tp - 1, rows + GAIN_ROWS, channels), jnp.bfloat16),
            pltpu.VMEM((tp - 1,) + weight.shape, jnp.bfloat16),
            pltpu.SemaphoreType.DMA((COPIES,)),
            pltpu.SemaphoreType.DMA((COPIES,)),
        ],
        compiler_params=pltpu.CompilerParams(
            collective_id=0, has_side_effects=True, vmem_limit_bytes=48 * 2**20
        ),
    )(outer, inner, values, taps, gain, weight, residual_in, moe_gain, near, far, both, down)


def ffn_kernel(x_ref, y_ref, wx_ref, wy_ref, own_both, own_down, both_ref, down_ref, x_out, y_out, x_acc, y_acc):
    step = pl.program_id(0)
    cuts, units, width = own_down.shape

    def part(rows_ref, w_ref, both, down):
        rows = rows_ref[...]
        hidden = []
        for cut in range(cuts):
            act = jnp.dot(rows, both[cut], preferred_element_type=jnp.float32)
            gated = jax.nn.silu(act[:, :units]) * act[:, units:]
            hidden.append((w_ref[0] * gated).astype(jnp.bfloat16))
        hidden = jnp.concatenate(hidden, axis=1)
        return jnp.dot(hidden, down[...].reshape(cuts * units, width), preferred_element_type=jnp.float32)

    tokens = ((x_ref, wx_ref, x_out, x_acc), (y_ref, wy_ref, y_out, y_acc))

    @pl.when(step == 0)
    def _():
        for rows_ref, w_ref, _, acc_ref in tokens:
            acc_ref[...] = part(rows_ref, w_ref, own_both, own_down)

    @pl.when(step > 0)
    def _():
        for rows_ref, w_ref, _, acc_ref in tokens:
            acc_ref[...] += part(rows_ref, w_ref, both_ref.at[0], down_ref.at[0])

    @pl.when(step == pl.num_programs(0) - 1)
    def _():
        for _, _, out_ref, acc_ref in tokens:
            out_ref[...] = acc_ref[...].astype(out_ref.dtype)


def weighted_experts(x, y, wx, wy, own_both, own_down, both, down):
    rows, width = x.shape
    cuts, units, _ = own_down.shape
    experts = wx.shape[0]
    full = pl.BlockSpec((rows, width), lambda e: (0, 0))
    scale = pl.BlockSpec((1, rows, 1), lambda e: (e, 0, 0))
    whole = lambda a: pl.BlockSpec(a.shape, lambda e: (0, 0, 0))
    other = lambda a: pl.BlockSpec((1,) + a.shape[1:], lambda e: (jnp.maximum(e - 1, 0), 0, 0, 0))
    return pl.pallas_call(
        ffn_kernel,
        grid=(experts,),
        in_specs=[full, full, scale, scale, whole(own_both), whole(own_down), other(both), other(down)],
        out_specs=[full, full],
        out_shape=[
            jax.ShapeDtypeStruct((rows, width), jnp.float32),
            jax.ShapeDtypeStruct((rows, width), jnp.bfloat16),
        ],
        scratch_shapes=[pltpu.VMEM((rows, width), jnp.float32)] * 2,
        compiler_params=pltpu.CompilerParams(
            dimension_semantics=("arbitrary",), vmem_limit_bytes=44 * 2**20
        ),
        cost_estimate=pl.CostEstimate(
            flops=12 * rows * width * units * cuts * experts,
            bytes_accessed=6 * cuts * experts * width * units + 12 * rows * width,
            transcendentals=2 * rows * units * cuts * experts,
        ),
    )(x, y, wx, wy, own_both, own_down, both, down)


def half_slice(
    residual_in,
    gate_outer,
    gate_inner,
    conv_input,
    conv_taps,
    norm_gain,
    out_weight,
    moe_gain,
    expert_ids,
    group_prob,
    route_prob,
    expert_gate,
    expert_up,
    expert_down,
):
    sp, tp = lax.axis_size("sp"), lax.axis_size("tp")
    half, lanes = sp // 2, tp // 2
    sp_me, tp_me = lax.axis_index("sp"), lax.axis_index("tp")
    rows, width = residual_in.shape
    core = [(i, i ^ 1) for i in range(tp)]
    cross = [(i, (i + half) % sp) for i in range(sp)]

    units = expert_gate.shape[2] // tp
    first = (tp_me % 2) * lanes * units
    cut = lambda a, start, axis: lax.dynamic_slice_in_dim(a, first + start, units, axis)
    own_both, own_down = [], []
    for piece in range(lanes):
        start = piece * units
        own_both += [cut(expert_gate, start, 2), cut(expert_up, start, 2)]
        own_down.append(cut(expert_down, start, 1))
    own_both = jnp.concatenate(
        [jnp.concatenate(own_both[2 * p : 2 * p + 2], axis=2) for p in range(lanes)], axis=0
    )
    own_down = jnp.concatenate(own_down, axis=0)

    scale = group_prob[:, None] * route_prob / jnp.sum(route_prob, axis=1, keepdims=True)
    side = (sp_me % half) ^ jnp.arange(half, dtype=jnp.int32)
    near_of = (sp_me // half) * half + side
    far_of = (1 - sp_me // half) * half + side

    def dense(experts):
        return jnp.sum(jnp.where(expert_ids[None] == experts[:, None, None], scale[None], 0.0), axis=2)

    near, far = dense(near_of), dense(far_of)
    (
        residual, routed, across, beside, across_beside, near_beside, far, far_beside, both, down
    ) = mixer(
        gate_outer, gate_inner, conv_input, conv_taps, norm_gain[None], out_weight, residual_in,
        moe_gain[None], near, far, own_both, own_down,
    )
    column = lambda w: w[..., None]
    experts = functools.partial(
        weighted_experts, own_both=own_both, own_down=own_down, both=both, down=down
    )
    theirs, others = experts(across, across_beside, column(far), column(far_beside))
    theirs = (theirs + lax.ppermute(others, "tp", core).astype(jnp.float32)).astype(jnp.bfloat16)
    back = lax.ppermute(theirs, "sp", cross)
    own, partner = experts(routed, beside, column(near), column(near_beside))
    own = own + lax.ppermute(partner, "tp", core).astype(jnp.float32)
    return (residual.astype(jnp.float32) + own + back.astype(jnp.float32)).astype(jnp.bfloat16)


def exchange_slots(
    residual_in,
    gate_outer,
    gate_inner,
    conv_input,
    conv_taps,
    norm_gain,
    out_weight,
    moe_gain,
    expert_ids,
    group_prob,
    route_prob,
    expert_gate,
    expert_up,
    expert_down,
):
    seq_rows, channels = conv_input.shape
    taps_count = conv_taps.shape[0]
    inner = gate_inner.astype(jnp.float32) * conv_input.astype(jnp.float32)
    earlier = from_behind(inner[seq_rows - (taps_count - 1) :], "sp", 1)
    padded = jnp.concatenate([earlier, inner], axis=0)
    tap_f = conv_taps.astype(jnp.float32)
    filtered = jnp.zeros((seq_rows, channels), jnp.float32)
    for offset in range(taps_count):
        filtered = filtered + tap_f[offset][None, :] * padded[offset : offset + seq_rows]
    mixed_out = (gate_outer.astype(jnp.float32) * filtered).astype(jnp.bfloat16)
    gathered = lax.all_to_all(mixed_out, "tp", split_axis=0, concat_axis=1, tiled=True)
    full_weight, full_gain = (
        lax.all_gather(out_weight, "tp", axis=0, tiled=True),
        lax.all_gather(norm_gain, "tp", axis=0, tiled=True),
    )
    normed = rms_norm(gathered, full_gain).astype(jnp.bfloat16)
    projected = jnp.dot(normed, full_weight, preferred_element_type=jnp.float32)
    residual = (residual_in.astype(jnp.float32) + projected).astype(jnp.bfloat16)
    routed_in = rms_norm(residual, moe_gain).astype(jnp.bfloat16)
    tok_rows, width = routed_in.shape
    top_count = expert_ids.shape[1]
    local_count = expert_gate.shape[0]
    group_count = lax.axis_size("sp")
    experts_all = local_count * group_count
    capacity = 2 * tok_rows * top_count // experts_all
    slots = tok_rows * top_count
    flat_e = expert_ids.reshape(-1)
    one_hot = (flat_e[:, None] == jnp.arange(experts_all, dtype=jnp.int32)[None, :]).astype(
        jnp.int32
    )
    slot_rank = jnp.sum((jnp.cumsum(one_hot, axis=0) - 1) * one_hot, axis=1)
    owner_dev = flat_e // local_count
    local_slot = flat_e % local_count
    position = (local_slot * group_count + owner_dev) * capacity + slot_rank
    source_slot = (
        jnp.full((experts_all * capacity,), slots, jnp.int32)
        .at[position]
        .set(jnp.arange(slots, dtype=jnp.int32))
    )
    rows_pad = jnp.concatenate([routed_in, jnp.zeros((1, width), jnp.bfloat16)], axis=0)
    outgoing = rows_pad[source_slot // top_count].reshape(local_count, group_count, capacity, width)
    arrived = lax.all_to_all(outgoing, "sp", split_axis=1, concat_axis=1, tiled=True)
    gate_act = jnp.einsum(
        "esrd,edf->esrf", arrived, expert_gate, preferred_element_type=jnp.float32
    )
    up_act = jnp.einsum("esrd,edf->esrf", arrived, expert_up, preferred_element_type=jnp.float32)
    hidden = (jax.nn.silu(gate_act) * up_act).astype(jnp.bfloat16)
    result = jnp.einsum(
        "esrf,efd->esrd", hidden, expert_down, preferred_element_type=jnp.float32
    ).astype(jnp.bfloat16)
    returned = lax.all_to_all(result, "sp", split_axis=1, concat_axis=1, tiled=True)
    slot_out = returned.reshape(-1, width)[position].reshape(tok_rows, top_count, width)
    weights = group_prob[:, None] * route_prob / jnp.sum(route_prob, axis=1, keepdims=True)
    expert_sum = jnp.sum(slot_out.astype(jnp.float32) * weights[:, :, None], axis=1)
    return (residual.astype(jnp.float32) + expert_sum).astype(jnp.bfloat16)


def solution(mesh):
    in_specs = (
        P(("sp", "tp"), None),
        P("sp", "tp"),
        P("sp", "tp"),
        P("sp", "tp"),
        P(None, "tp"),
        P("tp"),
        P("tp", None),
        P(),
        P(("sp", "tp"), None),
        P(("sp", "tp")),
        P(("sp", "tp"), None),
        P("sp", None, None),
        P("sp", None, None),
        P("sp", None, None),
    )
    out_specs = P(("sp", "tp"), None)
    def body(*args):
        gate, outer = args[11], args[1]
        sp, tp = mesh.shape["sp"], mesh.shape["tp"]
        gathered = 3 * gate.size * gate.dtype.itemsize * sp // 4
        pairs = gate.shape[0] == 1 and sp == 8 and tp == 4
        sized = gate.shape[2] % (128 * tp) == 0 and outer.shape[0] % (16 * tp) == 0
        if pairs and sized and gathered <= GATHER_BYTES:
            return half_slice(*args)
        return exchange_slots(*args)

    return jax.shard_map(body, mesh=mesh, in_specs=in_specs, out_specs=out_specs, check_vma=False)
```

```python
import functools
import jax
import jax.numpy as jnp
from jax import lax
from jax.experimental import pallas as pl
from jax.experimental.pallas import tpu as pltpu
from jax.sharding import PartitionSpec as P


MESH = pl.DeviceIdType.MESH
EPSILON = 1e-06


def from_behind(shard, axis, by):
    devices = lax.axis_size(axis)
    pairs = [(i, i + by) for i in range(devices) if 0 <= i + by < devices]
    return lax.ppermute(shard, axis, pairs)


def rms_norm(values, gain):
    floats = values.astype(jnp.float32)
    factor = lax.rsqrt(jnp.mean(floats * floats, axis=-1, keepdims=True) + EPSILON)
    return floats * factor * gain.astype(jnp.float32)


GATHER_BYTES = 26 * 2**20
GAIN_ROWS = 16
HALO_ROWS = 16


def mixer_kernel(
    outer_ref, inner_ref, input_ref, taps_ref, gain_ref, weight_ref, residual_ref, moe_ref, near_ref, far_ref,
    both_ref, down_ref,
    residual_out, routed_out, across_out, beside_out, across_beside_out,
    near_beside_out, far_out, far_beside_out, both_out, down_out,
    halo, sent, got, weights, send_sem, recv_sem,
):
    sp, tp = lax.axis_index("sp"), lax.axis_index("tp")
    sp_size, tp_size = lax.axis_size("sp"), lax.axis_size("tp")
    core_bit = 1 - 2 * (tp % 2)
    line_bit = 2 - 4 * ((tp // 2) % 2)
    lanes = [tp, tp + core_bit, tp + line_bit, tp + line_bit + core_bit]
    core, line = (sp, lanes[1]), (sp, lanes[2])
    x_peer = (sp + 1 - 2 * (sp % 2), tp)
    z_peer = (sp + 2 - 4 * ((sp // 2) % 2), tp)
    cross = ((sp + sp_size // 2) % sp_size, tp)
    after, before = ((sp + 1) % sp_size, tp), ((sp + sp_size - 1) % sp_size, tp)
    peers = [core, line, (sp, lanes[3]), x_peer, z_peer, cross, after, before]

    barrier = pltpu.get_barrier_semaphore()
    for peer in peers:
        pl.semaphore_signal(barrier, inc=1, device_id=peer, device_id_type=MESH)
    pl.semaphore_wait(barrier, len(peers))

    started = []

    def send(source, target, peer):
        number = len(started)
        copy = pltpu.make_async_remote_copy(
            src_ref=source, dst_ref=target, send_sem=send_sem.at[number], recv_sem=recv_sem.at[number],
            device_id=peer, device_id_type=MESH,
        )
        copy.start()
        started.append(copy)
        return copy

    full = inner_ref.shape[0]
    halos = [
        send(inner_ref.at[pl.ds(full - HALO_ROWS, HALO_ROWS)], halo.at[0], after),
        send(input_ref.at[pl.ds(full - HALO_ROWS, HALO_ROWS)], halo.at[1], after),
    ]
    weight_line = send(weight_ref, weights.at[1], line)
    weight_core = send(weight_ref, weights.at[0], core)

    def pieces(source_both, source_down, slot, piece, peer):
        return [
            send(source_both, both_out.at[slot, piece], peer),
            send(source_down, down_out.at[slot, piece], peer),
        ]

    mine = (tp // 2) % 2
    rest = 1 - mine
    x_first = pieces(both_ref.at[mine], down_ref.at[mine], 0, mine, x_peer)
    z_first = pieces(both_ref.at[mine], down_ref.at[mine], 1, mine, z_peer)
    x_second = pieces(both_ref.at[rest], down_ref.at[rest], 0, rest, x_peer)
    near_copy = send(near_ref, near_beside_out, core)
    far_copy = send(far_ref, far_out, cross)

    for copy in halos:
        copy.wait_recv()
    rows = residual_ref.shape[0]
    taps = taps_ref[...].astype(jnp.float32)
    count = taps.shape[0]
    exchanged = []
    for step in (2, 3, 1, 0):
        block = lanes[step]
        first = pl.multiple_of(block * rows, rows)
        inner = inner_ref[pl.ds(first, rows)].astype(jnp.float32) * input_ref[pl.ds(first, rows)].astype(jnp.float32)
        back = pl.multiple_of(jnp.maximum(block * rows - HALO_ROWS, 0), HALO_ROWS)
        behind = inner_ref[pl.ds(back, HALO_ROWS)].astype(jnp.float32) * input_ref[pl.ds(back, HALO_ROWS)].astype(jnp.float32)
        outside = halo[0].astype(jnp.float32) * halo[1].astype(jnp.float32)
        outside = jnp.where(sp == 0, 0.0, outside)
        behind = jnp.where(block == 0, outside, behind)
        padded = jnp.concatenate([behind, inner], axis=0)
        filtered = jnp.zeros_like(inner)
        for offset in range(count):
            start = HALO_ROWS - (count - 1) + offset
            filtered = filtered + taps[offset][None, :] * padded[start : start + rows]
        mixed = (outer_ref[pl.ds(first, rows)].astype(jnp.float32) * filtered).astype(jnp.bfloat16)
        sent[step, :rows] = mixed
        sent[step, rows:] = jnp.broadcast_to(gain_ref[...], (GAIN_ROWS, mixed.shape[1]))
        if step > 0:
            exchanged.append(send(sent.at[step], got.at[step - 1], (sp, block)))

    for copy in exchanged:
        copy.wait_recv()
    blocks = [sent.at[0], got.at[0], got.at[1], got.at[2]]
    total = jnp.zeros((rows, 1), jnp.float32)
    for block in blocks:
        values = block[:rows].astype(jnp.float32)
        total = total + jnp.sum(values * values, axis=1, keepdims=True)
    factor = lax.rsqrt(total / (tp_size * inner_ref.shape[1]) + EPSILON)

    def normed(block):
        gain = block[rows:][:1].astype(jnp.float32)
        return (block[:rows].astype(jnp.float32) * factor * gain).astype(jnp.bfloat16)

    weight_line.wait_recv()
    weight_both = send(weights.at[1], weights.at[2], core)
    far_copy.wait_recv()
    far_beside = send(far_out, far_beside_out, core)
    weight_core.wait_recv()
    out = residual_ref[...].astype(jnp.float32)
    out = out + jnp.dot(normed(blocks[0]), weight_ref[...], preferred_element_type=jnp.float32)
    out = out + jnp.dot(normed(blocks[1]), weights[0], preferred_element_type=jnp.float32)
    out = out + jnp.dot(normed(blocks[2]), weights[1], preferred_element_type=jnp.float32)
    weight_both.wait_recv()
    out = out + jnp.dot(normed(blocks[3]), weights[2], preferred_element_type=jnp.float32)
    residual = out.astype(jnp.bfloat16)
    residual_out[...] = residual
    floats = residual.astype(jnp.float32)
    mean = jnp.mean(floats * floats, axis=1, keepdims=True)
    routed = floats * lax.rsqrt(mean + EPSILON) * moe_ref[...].astype(jnp.float32)
    routed_out[...] = routed.astype(jnp.bfloat16)

    beside = send(routed_out, beside_out, core)
    for copy in z_first:
        copy.wait_recv()
    z_second = pieces(both_out.at[1, mine], down_out.at[1, mine], 1, mine, line)
    for copy in x_first:
        copy.wait_recv()
    diagonal = pieces(both_out.at[0, mine], down_out.at[0, mine], 2, mine, z_peer)
    across = send(routed_out, across_out, cross)
    for copy in z_second:
        copy.wait_recv()
    last_down = send(down_out.at[1, rest], down_out.at[2, rest], x_peer)
    for copy in diagonal:
        copy.wait_recv()
    last_both = send(both_out.at[2, mine], both_out.at[2, mine], line)
    across.wait_recv()
    across_beside = send(across_out, across_beside_out, core)
    for copy in x_second + [near_copy, far_beside, beside, last_down, last_both, across_beside]:
        copy.wait_recv()
    for copy in started:
        copy.wait_send()


COPIES = 26


def mixer(outer, inner, values, taps, gain, weight, residual_in, moe_gain, near, far, both, down):
    rows, width = residual_in.shape
    channels = outer.shape[1]
    tp = lax.axis_size("tp")
    vmem = pl.BlockSpec(memory_space=pltpu.VMEM)
    hbm = pl.BlockSpec(memory_space=pl.ANY)
    tokens = jax.ShapeDtypeStruct((rows, width), jnp.bfloat16)
    scale = jax.ShapeDtypeStruct(near.shape, near.dtype)
    return pl.pallas_call(
        mixer_kernel,
        in_specs=[vmem] * 10 + [hbm] * 2,
        out_specs=[vmem, vmem, hbm, hbm, hbm, vmem, vmem, vmem, hbm, hbm],
        out_shape=[tokens] * 5
        + [scale] * 3
        + [jax.ShapeDtypeStruct((3,) + a.shape, a.dtype) for a in (both, down)],
        scratch_shapes=[
            pltpu.VMEM((2, HALO_ROWS, channels), jnp.bfloat16),
            pltpu.VMEM((tp, rows + GAIN_ROWS, channels), jnp.bfloat16),
            pltpu.VMEM((tp - 1, rows + GAIN_ROWS, channels), jnp.bfloat16),
            pltpu.VMEM((tp - 1,) + weight.shape, jnp.bfloat16),
            pltpu.SemaphoreType.DMA((COPIES,)),
            pltpu.SemaphoreType.DMA((COPIES,)),
        ],
        compiler_params=pltpu.CompilerParams(
            collective_id=0, has_side_effects=True, vmem_limit_bytes=48 * 2**20
        ),
    )(outer, inner, values, taps, gain, weight, residual_in, moe_gain, near, far, both, down)


def ffn_kernel(x_ref, y_ref, wx_ref, wy_ref, own_both, own_down, both_ref, down_ref, x_out, y_out, x_acc, y_acc):
    step = pl.program_id(0)
    cuts, units, width = own_down.shape

    def part(rows_ref, w_ref, both, down):
        rows = rows_ref[...]
        scale = w_ref[pl.ds(step, 1), :].T
        hidden = []
        for cut in range(cuts):
            act = jnp.dot(rows, both[cut], preferred_element_type=jnp.float32)
            gated = jax.nn.silu(act[:, :units]) * act[:, units:]
            hidden.append((scale * gated).astype(jnp.bfloat16))
        hidden = jnp.concatenate(hidden, axis=1)
        return jnp.dot(hidden, down[...].reshape(cuts * units, width), preferred_element_type=jnp.float32)

    tokens = ((x_ref, wx_ref, x_out, x_acc), (y_ref, wy_ref, y_out, y_acc))

    @pl.when(step == 0)
    def _():
        for rows_ref, w_ref, _, acc_ref in tokens:
            acc_ref[...] = part(rows_ref, w_ref, own_both, own_down)

    @pl.when(step > 0)
    def _():
        for rows_ref, w_ref, _, acc_ref in tokens:
            acc_ref[...] += part(rows_ref, w_ref, both_ref.at[0], down_ref.at[0])

    @pl.when(step == pl.num_programs(0) - 1)
    def _():
        for _, _, out_ref, acc_ref in tokens:
            out_ref[...] = acc_ref[...].astype(out_ref.dtype)


def weighted_experts(x, y, wx, wy, own_both, own_down, both, down):
    rows, width = x.shape
    cuts, units, _ = own_down.shape
    experts = wx.shape[0]
    full = pl.BlockSpec((rows, width), lambda e: (0, 0))
    scale = pl.BlockSpec(wx.shape, lambda e: (0, 0))
    whole = lambda a: pl.BlockSpec(a.shape, lambda e: (0, 0, 0))
    other = lambda a: pl.BlockSpec((1,) + a.shape[1:], lambda e: (jnp.maximum(e - 1, 0), 0, 0, 0))
    return pl.pallas_call(
        ffn_kernel,
        grid=(experts,),
        in_specs=[full, full, scale, scale, whole(own_both), whole(own_down), other(both), other(down)],
        out_specs=[full, full],
        out_shape=[
            jax.ShapeDtypeStruct((rows, width), jnp.float32),
            jax.ShapeDtypeStruct((rows, width), jnp.bfloat16),
        ],
        scratch_shapes=[pltpu.VMEM((rows, width), jnp.float32)] * 2,
        compiler_params=pltpu.CompilerParams(
            dimension_semantics=("arbitrary",), vmem_limit_bytes=60 * 2**20
        ),
        cost_estimate=pl.CostEstimate(
            flops=12 * rows * width * units * cuts * experts,
            bytes_accessed=6 * cuts * experts * width * units + 12 * rows * width,
            transcendentals=2 * rows * units * cuts * experts,
        ),
    )(x, y, wx, wy, own_both, own_down, both, down)


def half_slice(
    residual_in,
    gate_outer,
    gate_inner,
    conv_input,
    conv_taps,
    norm_gain,
    out_weight,
    moe_gain,
    expert_ids,
    group_prob,
    route_prob,
    expert_gate,
    expert_up,
    expert_down,
):
    sp, tp = lax.axis_size("sp"), lax.axis_size("tp")
    half, lanes = sp // 2, tp // 2
    sp_me, tp_me = lax.axis_index("sp"), lax.axis_index("tp")
    core = [(i, i ^ 1) for i in range(tp)]
    cross = [(i, (i + half) % sp) for i in range(sp)]

    units = expert_gate.shape[2] // tp
    first = (tp_me % 2) * lanes * units
    cut = lambda a, start, axis: lax.dynamic_slice_in_dim(a, first + start, units, axis)
    own_both, own_down = [], []
    for piece in range(lanes):
        start = piece * units
        own_both += [cut(expert_gate, start, 2), cut(expert_up, start, 2)]
        own_down.append(cut(expert_down, start, 1))
    own_both = jnp.concatenate(
        [jnp.concatenate(own_both[2 * p : 2 * p + 2], axis=2) for p in range(lanes)], axis=0
    )
    own_down = jnp.concatenate(own_down, axis=0)

    scale = group_prob[:, None] * route_prob / jnp.sum(route_prob, axis=1, keepdims=True)
    side = (sp_me % half) ^ jnp.arange(half, dtype=jnp.int32)
    near_of = (sp_me // half) * half + side
    far_of = (1 - sp_me // half) * half + side

    def dense(experts):
        return jnp.sum(jnp.where(expert_ids[None] == experts[:, None, None], scale[None], 0.0), axis=2)

    near, far = dense(near_of), dense(far_of)
    (
        residual, routed, across, beside, across_beside, near_beside, far, far_beside, both, down
    ) = mixer(
        gate_outer, gate_inner, conv_input, conv_taps, norm_gain[None], out_weight, residual_in,
        moe_gain[None], near, far, own_both, own_down,
    )
    experts = functools.partial(
        weighted_experts, own_both=own_both, own_down=own_down, both=both, down=down
    )
    theirs, others = experts(across, across_beside, far, far_beside)
    theirs = (theirs + lax.ppermute(others, "tp", core).astype(jnp.float32)).astype(jnp.bfloat16)
    near, theirs = lax.optimization_barrier((near, theirs))
    back = lax.ppermute(theirs, "sp", cross)
    own, partner = experts(routed, beside, near, near_beside)
    own = own + lax.ppermute(partner, "tp", core).astype(jnp.float32)
    return (residual.astype(jnp.float32) + own + back.astype(jnp.float32)).astype(jnp.bfloat16)


def exchange_slots(
    residual_in,
    gate_outer,
    gate_inner,
    conv_input,
    conv_taps,
    norm_gain,
    out_weight,
    moe_gain,
    expert_ids,
    group_prob,
    route_prob,
    expert_gate,
    expert_up,
    expert_down,
):
    seq_rows, channels = conv_input.shape
    taps_count = conv_taps.shape[0]
    inner = gate_inner.astype(jnp.float32) * conv_input.astype(jnp.float32)
    earlier = from_behind(inner[seq_rows - (taps_count - 1) :], "sp", 1)
    padded = jnp.concatenate([earlier, inner], axis=0)
    tap_f = conv_taps.astype(jnp.float32)
    filtered = jnp.zeros((seq_rows, channels), jnp.float32)
    for offset in range(taps_count):
        filtered = filtered + tap_f[offset][None, :] * padded[offset : offset + seq_rows]
    mixed_out = (gate_outer.astype(jnp.float32) * filtered).astype(jnp.bfloat16)
    gathered = lax.all_to_all(mixed_out, "tp", split_axis=0, concat_axis=1, tiled=True)
    full_weight, full_gain = (
        lax.all_gather(out_weight, "tp", axis=0, tiled=True),
        lax.all_gather(norm_gain, "tp", axis=0, tiled=True),
    )
    normed = rms_norm(gathered, full_gain).astype(jnp.bfloat16)
    projected = jnp.dot(normed, full_weight, preferred_element_type=jnp.float32)
    residual = (residual_in.astype(jnp.float32) + projected).astype(jnp.bfloat16)
    routed_in = rms_norm(residual, moe_gain).astype(jnp.bfloat16)
    tok_rows, width = routed_in.shape
    top_count = expert_ids.shape[1]
    local_count = expert_gate.shape[0]
    group_count = lax.axis_size("sp")
    experts_all = local_count * group_count
    capacity = 2 * tok_rows * top_count // experts_all
    slots = tok_rows * top_count
    flat_e = expert_ids.reshape(-1)
    one_hot = (flat_e[:, None] == jnp.arange(experts_all, dtype=jnp.int32)[None, :]).astype(
        jnp.int32
    )
    slot_rank = jnp.sum((jnp.cumsum(one_hot, axis=0) - 1) * one_hot, axis=1)
    owner_dev = flat_e // local_count
    local_slot = flat_e % local_count
    position = (local_slot * group_count + owner_dev) * capacity + slot_rank
    source_slot = (
        jnp.full((experts_all * capacity,), slots, jnp.int32)
        .at[position]
        .set(jnp.arange(slots, dtype=jnp.int32))
    )
    rows_pad = jnp.concatenate([routed_in, jnp.zeros((1, width), jnp.bfloat16)], axis=0)
    outgoing = rows_pad[source_slot // top_count].reshape(local_count, group_count, capacity, width)
    arrived = lax.all_to_all(outgoing, "sp", split_axis=1, concat_axis=1, tiled=True)
    gate_act = jnp.einsum(
        "esrd,edf->esrf", arrived, expert_gate, preferred_element_type=jnp.float32
    )
    up_act = jnp.einsum("esrd,edf->esrf", arrived, expert_up, preferred_element_type=jnp.float32)
    hidden = (jax.nn.silu(gate_act) * up_act).astype(jnp.bfloat16)
    result = jnp.einsum(
        "esrf,efd->esrd", hidden, expert_down, preferred_element_type=jnp.float32
    ).astype(jnp.bfloat16)
    returned = lax.all_to_all(result, "sp", split_axis=1, concat_axis=1, tiled=True)
    slot_out = returned.reshape(-1, width)[position].reshape(tok_rows, top_count, width)
    weights = group_prob[:, None] * route_prob / jnp.sum(route_prob, axis=1, keepdims=True)
    expert_sum = jnp.sum(slot_out.astype(jnp.float32) * weights[:, :, None], axis=1)
    return (residual.astype(jnp.float32) + expert_sum).astype(jnp.bfloat16)


def solution(mesh):
    in_specs = (
        P(("sp", "tp"), None),
        P("sp", "tp"),
        P("sp", "tp"),
        P("sp", "tp"),
        P(None, "tp"),
        P("tp"),
        P("tp", None),
        P(),
        P(("sp", "tp"), None),
        P(("sp", "tp")),
        P(("sp", "tp"), None),
        P("sp", None, None),
        P("sp", None, None),
        P("sp", None, None),
    )
    out_specs = P(("sp", "tp"), None)
    sp, tp = mesh.shape["sp"], mesh.shape["tp"]

    def body(*args):
        gate, outer = args[11], args[1]
        gathered = 3 * gate.size * gate.dtype.itemsize * sp // 4
        pairs = gate.shape[0] == 1 and sp == 8 and tp == 4
        sized = gate.shape[2] % (128 * tp) == 0 and outer.shape[0] % (16 * tp) == 0
        if pairs and sized and gathered <= GATHER_BYTES:
            return half_slice(*args)
        return exchange_slots(*args)

    return jax.shard_map(body, mesh=mesh, in_specs=in_specs, out_specs=out_specs, check_vma=False)
```
